256 devices in a mesh: sp: 32 (over z, y), tp: 8 (over x, core).
Axes of the slice: x: 4, y: 4, z: 8, core: 2. Of those that a mesh axis runs over, the one named last changes fastest.
Arguments:
- activations: bfloat16 [14336, 2048], P(('sp', 'tp')), may hold values from -27.5 to 27.5
- query_weight: bfloat16 [2048, 2048], P(None, 'tp'), may hold values from -0.088388348 to 0.088388348
- key_weight: bfloat16 [2048, 2048], P(None, 'tp'), may hold values from -0.088388348 to 0.088388348
- value_weight: bfloat16 [2048, 2048], P(None, 'tp'), may hold values from -0.125 to 0.125
- out_weight: bfloat16 [2048, 2048], P('tp'), may hold values from -0.125 to 0.125
- lambdas: float32 [8], P('tp'), may hold values from 0.3 to 0.8
- head_gain: float32 [256], replicated, may hold values from 0.1 to 1.9
Outputs:
- mixed: bfloat16 [14336, 2048], P(('sp', 'tp'))
The draws below stay inside these ranges and needn't reach their ends.
All inputs are finite; a program needn't handle non-finite values.
Results may differ from the reference program's by a relative error of at most 0.014.
Values may be sent and summed in bfloat16 or wider, within the bound.
A program may use at most 128 MiB of HBM per device.

```python
import jax
import jax.numpy as jnp
from jax import lax

D = 2048
HEADS = 8
HEAD = 128
VALUE = 256
TOK_DEV = 448
SEQ = 14336
N_TP = 8


def draw_activations(key, part):
    noise_base = jnp.clip(jax.random.normal(jax.random.fold_in(key, 1), (SEQ, D), jnp.float32), -4.0, 4.0)
    block_means = jax.random.uniform(jax.random.fold_in(key, 2), (SEQ // TOK_DEV, D), jnp.float32, -1.5, 1.5)
    result = noise_base + jnp.repeat(block_means, TOK_DEV, axis=0)
    return result.astype(jnp.bfloat16)


def paired_weights(key):
    bound_value = 4.0 * D ** (-0.5)
    first_draw = jax.random.normal(jax.random.fold_in(key, 11), (D, HEADS * 2 * HEAD), jnp.float32) * D ** (-0.5)
    second = jax.random.normal(jax.random.fold_in(key, 12), (D, HEADS * 2 * HEAD), jnp.float32) * D ** (-0.5)
    return (first_draw, second, bound_value)


def draw_query_weight(key, part):
    first_draw, second, bound_value = paired_weights(key)
    return jnp.clip(first_draw, -bound_value, bound_value).astype(jnp.bfloat16)


def draw_key_weight(key, part):
    first_draw, second, bound_value = paired_weights(key)
    mixed_draw = second
    return jnp.clip(mixed_draw, -bound_value, bound_value).astype(jnp.bfloat16)


def level_of(key, shape, shards, least, largest):
    gain = 1.0
    for dim, blocks in shards:
        draws = jax.random.uniform(jax.random.fold_in(jax.random.fold_in(key, 6), dim), (blocks,), jnp.float32, least / len(shards), largest / len(shards))
        gain = gain * jnp.repeat(jnp.exp(draws), shape[dim] // blocks).reshape((-1,) + (1,) * (len(shape) - 1 - dim))
    return gain


def bell_draw(stream_key, dims, deviation, reach, split=(), kind=jnp.bfloat16):
    values = jax.random.normal(stream_key, dims, jnp.float32) * deviation
    if len(split) > 0:
        values = level_of(stream_key, dims, split, -0.22, 0.18) * values
    return jnp.clip(values, min=-reach, max=reach).astype(kind)


def setup_inputs(seed: int = 0) -> dict:
    key_of = jax.random.split(jax.random.key(seed), 8)
    activations = draw_activations(jax.random.fold_in(key_of[7], 71), 0)
    query_weight = draw_query_weight(jax.random.fold_in(key_of[7], 71), 0)
    key_weight = draw_key_weight(jax.random.fold_in(key_of[7], 71), 0)
    value_weight = bell_draw(key_of[3], (D, HEADS * VALUE), D ** -0.5, 0.125, ((1, 8),))
    out_weight = bell_draw(key_of[4], (HEADS * VALUE, D), (HEADS * VALUE) ** -0.5, 0.125, ((0, 8),))
    lambdas = jnp.clip(0.3 + 0.5 * jax.random.uniform(key_of[5], (HEADS,), jnp.float32) ** level_of(key_of[5], (HEADS,), ((0, 8),), -0.2, 0.2), 0.3, 0.8)
    head_gain = jnp.clip(1.0 + 0.18 * jax.random.normal(key_of[6], (VALUE,), jnp.float32), 0.1, 1.9)
    return dict(activations=activations, query_weight=query_weight, key_weight=key_weight, value_weight=value_weight, out_weight=out_weight, lambdas=lambdas, head_gain=head_gain)


norm_floor = 0.02

def reference(activations, query_weight, key_weight, value_weight, out_weight, lambdas, head_gain):
    queries = jnp.dot(activations, query_weight, preferred_element_type=jnp.float32).astype(jnp.bfloat16)
    key_rows = jnp.dot(activations, key_weight, preferred_element_type=jnp.float32).astype(jnp.bfloat16)
    value_rows = jnp.dot(activations, value_weight, preferred_element_type=jnp.float32).astype(jnp.bfloat16)
    queries = queries.reshape(SEQ, HEADS, 2, HEAD).transpose(1, 0, 2, 3)
    key_rows = key_rows.reshape(SEQ, HEADS, 2, HEAD).transpose(1, 0, 2, 3)
    value_rows = value_rows.reshape(SEQ, HEADS, VALUE).transpose(1, 0, 2)
    blocks = SEQ // TOK_DEV
    score_scale = HEAD ** (-0.5)
    key_pos = jnp.arange(SEQ, dtype=jnp.int32)

    def one_block(index):
        head_index = index // blocks
        block_index = index % blocks
        first_row = (block_index * TOK_DEV).astype(jnp.int32)
        query_rows = lax.dynamic_slice_in_dim(queries[head_index], first_row, TOK_DEV, 0).astype(jnp.float32)
        key_all = key_rows[head_index].astype(jnp.float32)
        value_all = value_rows[head_index].astype(jnp.float32)
        scores = jnp.einsum('qme,kme->mqk', query_rows, key_all) * score_scale
        query_pos = first_row + jnp.arange(TOK_DEV, dtype=jnp.int32)
        allowed = key_pos[None, :] <= query_pos[:, None]
        masked = jnp.where(allowed[None], scores, -jnp.inf)
        row_top = lax.optimization_barrier(jnp.max(masked, axis=-1, keepdims=True))
        exp_weights = jnp.where(allowed[None], jnp.exp(masked - row_top), 0.0)
        denominators = lax.optimization_barrier(jnp.sum(exp_weights, axis=-1))
        rounded = lax.optimization_barrier(exp_weights.astype(jnp.bfloat16)).astype(jnp.float32)
        weighted = jnp.einsum('mqk,kv->mqv', rounded, value_all)
        lambda_head = lambdas[head_index]
        combined = weighted[0] / denominators[0][:, None] - lambda_head * weighted[1] / denominators[1][:, None]
        inverse_rms = lax.rsqrt(lax.optimization_barrier(jnp.mean(combined * combined, axis=-1, keepdims=True)) + norm_floor)
        return (combined * inverse_rms * head_gain).astype(jnp.bfloat16)
    heads_out = lax.map(one_block, jnp.arange(HEADS * blocks, dtype=jnp.int32))
    heads_out = heads_out.reshape(HEADS, SEQ, VALUE).transpose(1, 0, 2).reshape(SEQ, HEADS * VALUE)
    group_width = HEADS // N_TP * VALUE
    totals = jnp.zeros((SEQ, D), jnp.float32)
    for group_index in range(N_TP):
        columns = heads_out[:, group_index * group_width:(group_index + 1) * group_width]
        weight_rows = out_weight[group_index * group_width:(group_index + 1) * group_width]
        partial_value = jnp.dot(columns, weight_rows, preferred_element_type=jnp.float32).astype(jnp.bfloat16)
        totals = totals + partial_value.astype(jnp.float32)
    return totals.astype(jnp.bfloat16)
```

```python
import functools
import math

import jax
import jax.numpy as jnp
from jax import lax
from jax.experimental import pallas as pl
from jax.experimental.pallas import tpu as pltpu
from jax.sharding import PartitionSpec as P

HEAD = 128
VALUE = 256
norm_floor = 0.02
very_low = -1e30
EXP_SCALE = HEAD ** (-0.5) * math.log2(math.e)
MESH = pl.DeviceIdType.MESH
F32 = jnp.float32
BF16 = jnp.bfloat16


def fused(X, Y, Z, TOK, D, R, QT, *refs):
    (
        x_hbm, wq_hbm, wk_hbm, wv_hbm, wo_hbm, lam_ref, gain_ref, out_ref,
        xg, wq, wk, wv, wo, proj, kv, qg, vt, acc, stats, part,
        y_relay, y_in, y_sum, hn, d_out, d_in, sx, x_relay, x_in, x_sum,
        load_sem, xa_send, xa_recv, dd_send, dd_recv, q_send, q_recv,
        zr_send, zr_recv, zl_send, zl_recv, st_send, st_recv,
        yr_send, yr_recv, do_send, do_recv, xr_send, xr_recv,
    ) = refs
    NT = Y * TOK // QT
    half = TOK // 2
    cols = D // 2
    reach = Z // 2

    sp = lax.axis_index("sp")
    tp = lax.axis_index("tp")
    z, y = sp // Y, lax.rem(sp, Y)
    x, c = tp // 2, lax.rem(tp, 2)
    x_up, x_down, x_far = lax.rem(x + 1, X), lax.rem(x + X - 1, X), lax.rem(x + X // 2, X)
    y_up, y_down, y_far = lax.rem(y + 1, Y), lax.rem(y + Y - 1, Y), lax.rem(y + Y // 2, Y)
    z_up, z_down = lax.rem(z + 1, Z), lax.rem(z + Z - 1, Z)
    other = 1 - c

    def at_x(xx, cc):
        return (sp, xx * 2 + cc)

    def at_y(yy):
        return (z * Y + yy, tp)

    def at_z(zz):
        return (zz * Y + y, tp)

    def remote(src, dst, send, recv, where):
        return pltpu.make_async_remote_copy(
            src_ref=src, dst_ref=dst, send_sem=send, recv_sem=recv, device_id=where, device_id_type=MESH
        )

    loads = [
        pltpu.make_async_copy(a, b, load_sem.at[i])
        for i, (a, b) in enumerate(
            ((x_hbm, xg.at[tp]), (wq_hbm, wq), (wk_hbm, wk), (wv_hbm, wv), (wo_hbm, wo))
        )
    ]
    for load in loads:
        load.start()

    peers = [at_x(x, other)]
    if X > 1:
        peers += [at_x(x_up, c), at_x(x_down, c)]
    if Y > 1:
        peers += [at_y(y_up), at_y(y_down), at_y(y_far)]
    if Z > 1:
        peers += [at_z(z_up), at_z(z_down)]
    barrier = pltpu.get_barrier_semaphore()
    for peer in peers:
        pl.semaphore_signal(barrier, inc=1, device_id=peer, device_id_type=MESH)
    pl.semaphore_wait(barrier, len(peers))

    def slot(xx, cc):
        return xx * 2 + cc

    def block_copy(index, send, recv, where):
        return remote(xg.at[index], xg.at[index], send, recv, where)

    loads[0].wait()
    xa = []
    if X > 1:
        xa = [
            block_copy(tp, xa_send.at[0], xa_recv.at[0], at_x(x_up, c)),
            block_copy(tp, xa_send.at[1], xa_recv.at[1], at_x(x_down, c)),
            block_copy(
                jnp.where(c == 0, slot(x_down, c), slot(x_up, c)),
                xa_send.at[2], xa_recv.at[2], at_x(jnp.where(c == 0, x_up, x_down), c),
            ),
        ]
    dd = [block_copy(tp, dd_send.at[0], dd_recv.at[0], at_x(x, other))]
    if X > 1:
        dd += [
            block_copy(slot(x_down, c), dd_send.at[1], dd_recv.at[1], at_x(x, other)),
            block_copy(slot(x_up, c), dd_send.at[2], dd_recv.at[2], at_x(x, other)),
            block_copy(slot(x_far, c), dd_send.at[3], dd_recv.at[3], at_x(x, other)),
        ]
    if X > 1:
        xa[0].start()
        xa[1].start()
    dd[0].start()
    for load in loads[1:4]:
        load.wait()

    def project(i, carry):
        if X > 1:

            @pl.when(i == 1)
            def _():
                dd[0].wait_recv()

            @pl.when(i == 2)
            def _():
                xa[0].wait_recv()
                xa[1].wait_recv()
                xa[2].start()
                dd[1].start()
                dd[2].start()

            @pl.when(i == 4)
            def _():
                dd[1].wait_recv()
                dd[2].wait_recv()

            @pl.when(i == 6)
            def _():
                xa[2].wait_recv()
                dd[3].start()

            @pl.when(i == 7)
            def _():
                dd[3].wait_recv()

            xx = jnp.where(i < 2, x, jnp.where(i >= 6, x_far, jnp.where(lax.rem(i, 2) == 0, x_down, x_up)))
            cc = jnp.where((i == 1) | (i == 4) | (i == 5) | (i == 7), other, c)
        else:

            @pl.when(i == 1)
            def _():
                dd[0].wait_recv()

            xx = x
            cc = jnp.where(i == 1, other, c)
        index = slot(xx, cc)
        rows = pl.ds(pl.multiple_of(index * R, 8), R)
        block = xg[index]
        for n, w in enumerate((wq, wk, wv)):
            proj[rows, n * 256 : (n + 1) * 256] = jnp.dot(block, w[...], preferred_element_type=F32)
        return carry

    lax.fori_loop(0, 2 * X, project, 0)
    kv[z] = proj[:, 256:768].astype(BF16)
    q_row = pl.multiple_of(y * TOK, 16)
    qg[pl.ds(q_row, TOK), :] = proj[:, 0:256].astype(BF16)

    def z_copy(right, s, k, origin):
        rows = pl.ds(pl.multiple_of(k * half, 16), half)
        piece = kv.at[origin, rows, :]
        if right:
            return remote(piece, piece, zr_send.at[s, k], zr_recv.at[s, k], at_z(z_up))
        return remote(piece, piece, zl_send.at[s, k], zl_recv.at[s, k], at_z(z_down))

    def right_origin(zz, s):
        return lax.rem(zz - s + Z, Z)

    def left_origin(zz, s):
        return lax.rem(zz + s, Z)

    def right_goes(zz, s, k):
        return (zz - s >= 0) & (zz + 1 < Z) & ((s < reach - 1) | ((s == reach - 1) & (k == 0)))

    def left_goes(zz, s, k):
        o = left_origin(zz, s)
        return (o < reach) & ((o < reach - 1) | (k == 1)) & ((s < reach - 1) | ((s == reach - 1) & (k == 1)))

    if Z > 1:
        for k in range(2):

            @pl.when(right_goes(z, 0, k))
            def _():
                z_copy(True, 0, k, z).start()

            @pl.when(left_goes(z, 0, k))
            def _():
                z_copy(False, 0, k, z).start()

    def q_copy(yy, part_no, n, where):
        piece = qg.at[pl.ds(pl.multiple_of(yy * TOK + part_no * half, 16), half), :]
        return remote(piece, piece, q_send.at[n], q_recv.at[n], where)

    if Y > 1:
        qc = [
            q_copy(y, 0, 0, at_y(y_up)),
            q_copy(y, 1, 1, at_y(y_up)),
            q_copy(y_down, 0, 2, at_y(y_up)),
            q_copy(y, 1, 3, at_y(y_down)),
            q_copy(y, 0, 4, at_y(y_down)),
            q_copy(y_up, 1, 5, at_y(y_down)),
        ]
        for n in (0, 3, 1, 4):
            qc[n].start()
        qc[0].wait_recv()
        qc[2].start()
        qc[3].wait_recv()
        qc[5].start()
        for n in (1, 4, 2, 5):
            qc[n].wait_recv()

    vt[:, 0:TOK] = jnp.transpose(kv[z, :, 256:512].astype(F32)).astype(BF16)

    def own_tile(t, carry):
        rows = pl.ds(pl.multiple_of(t * QT, 16), QT)
        key_pos = lax.broadcasted_iota(jnp.int32, (TOK, QT), 0) + y * TOK
        query_pos = lax.broadcasted_iota(jnp.int32, (TOK, QT), 1) + t * QT
        allowed = key_pos <= query_pos
        for m in range(2):
            lanes = slice(m * HEAD, (m + 1) * HEAD)
            s = lax.dot_general(
                kv[z, :, lanes], qg[rows, lanes], (((1,), (1,)), ((), ())), preferred_element_type=F32
            )
            s = jnp.where(allowed, s, very_low)
            top = jnp.maximum(jnp.max(s, axis=0, keepdims=True), very_low)
            p = jnp.where(allowed, jnp.exp2((s - top) * EXP_SCALE), 0.0)
            stats[t, m : m + 1, :] = top
            stats[t, 2 + m : 3 + m, :] = jnp.sum(p, axis=0, keepdims=True)
            acc[t, m] = jnp.dot(vt[:, 0:TOK], p.astype(BF16), preferred_element_type=F32)
        return carry

    lax.fori_loop(0, NT, own_tile, 0)

    def attend(origin, k):
        key_rows = pl.ds(pl.multiple_of(k * half, 16), half)
        vt[:, 0:half] = jnp.transpose(kv[origin, key_rows, 256:512].astype(F32)).astype(BF16)

        def tile(t, carry):
            rows = pl.ds(pl.multiple_of(t * QT, 16), QT)
            for m in range(2):
                lanes = slice(m * HEAD, (m + 1) * HEAD)
                s = lax.dot_general(
                    kv[origin, key_rows, lanes],
                    qg[rows, lanes],
                    (((1,), (1,)), ((), ())),
                    preferred_element_type=F32,
                )
                before = stats[t, m : m + 1, :]
                top = jnp.maximum(before, jnp.max(s, axis=0, keepdims=True))
                p = jnp.exp2((s - top) * EXP_SCALE)
                factor = jnp.exp2((before - top) * EXP_SCALE)
                stats[t, m : m + 1, :] = top
                stats[t, 2 + m : 3 + m, :] = stats[t, 2 + m : 3 + m, :] * factor + jnp.sum(
                    p, axis=0, keepdims=True
                )
                acc[t, m] = acc[t, m] * factor + jnp.dot(
                    vt[:, 0:half], p.astype(BF16), preferred_element_type=F32
                )
            return carry

        lax.fori_loop(0, NT, tile, 0)

    if Z > 1:

        def event(e, carry):
            s, k = e // 2, lax.rem(e, 2)
            from_left = (z >= 1) & right_goes(z - 1, s, k)
            from_right = left_goes(z_up, s, k)
            o_left = right_origin(z_down, s)
            o_right = left_origin(z_up, s)

            @pl.when(from_left)
            def _():
                z_copy(True, s, k, o_left).wait_recv()

            @pl.when(from_left & right_goes(z, s + 1, k))
            def _():
                z_copy(True, s + 1, k, o_left).start()

            @pl.when(from_right)
            def _():
                z_copy(False, s, k, o_right).wait_recv()

            @pl.when(from_right & left_goes(z, s + 1, k))
            def _():
                z_copy(False, s + 1, k, o_right).start()

            def side(i, carry2):
                o = jnp.where(i == 0, o_left, o_right)
                use = jnp.where(i == 0, from_left, from_right & (o_right < z))

                @pl.when(use)
                def _():
                    attend(o, k)

                return carry2

            lax.fori_loop(0, 2, side, 0)
            return carry

        lax.fori_loop(0, 2 * reach, event, 0)

    if Y > 1:
        sc = [
            remote(stats.at[pl.ds(0, NT)], stats.at[pl.ds((n + 1) * NT, NT)], st_send.at[n], st_recv.at[n], at_y(yy))
            for n, yy in enumerate((y_up, y_down, y_far))
        ]
        for copy in sc:
            copy.start()
        for copy in sc:
            copy.wait_recv()

    lam = lam_ref[0]

    def combine(t, carry):
        rows = pl.ds(pl.multiple_of(t * QT, 16), QT)
        shares = []
        for m in range(2):
            own_top = stats[t, m : m + 1, :]
            tops = [own_top]
            sums = [stats[t, 2 + m : 3 + m, :]]
            if Y > 1:
                for n in range(3):
                    tops.append(stats[(n + 1) * NT + t, m : m + 1, :])
                    sums.append(stats[(n + 1) * NT + t, 2 + m : 3 + m, :])
            top = functools.reduce(jnp.maximum, tops)
            total = functools.reduce(
                jnp.add, [s * jnp.exp2((a - top) * EXP_SCALE) for a, s in zip(tops, sums)]
            )
            shares.append(jnp.exp2((own_top - top) * EXP_SCALE) / total)
        joined = acc[t, 0] * shares[0] - acc[t, 1] * (shares[1] * lam)
        part[rows, :] = jnp.transpose(joined).astype(BF16)
        return carry

    lax.fori_loop(0, NT, combine, 0)

    def owned(yy, h):
        return pl.ds(pl.multiple_of(yy * TOK + h * half, 16), half)

    low, high = pl.ds(0, half), pl.ds(half, half)
    if Y > 1:
        yr = [
            remote(part.at[owned(y_far, 0), :], y_relay.at[0], yr_send.at[0], yr_recv.at[0], at_y(y_up)),
            remote(part.at[owned(y_far, 1), :], y_relay.at[1], yr_send.at[1], yr_recv.at[1], at_y(y_down)),
            remote(part.at[owned(y_up, 1), :], y_in.at[0, high, :], yr_send.at[2], yr_recv.at[2], at_y(y_up)),
            remote(part.at[owned(y_down, 0), :], y_in.at[1, low, :], yr_send.at[3], yr_recv.at[3], at_y(y_down)),
            remote(y_sum.at[0], y_in.at[0, low, :], yr_send.at[4], yr_recv.at[4], at_y(y_up)),
            remote(y_sum.at[1], y_in.at[1, high, :], yr_send.at[5], yr_recv.at[5], at_y(y_down)),
        ]
        for n in range(4):
            yr[n].start()
        yr[0].wait_recv()
        y_sum[0] = (part[owned(y_up, 0), :].astype(F32) + y_relay[0].astype(F32)).astype(BF16)
        yr[4].start()
        yr[1].wait_recv()
        y_sum[1] = (part[owned(y_down, 1), :].astype(F32) + y_relay[1].astype(F32)).astype(BF16)
        yr[5].start()
        for n in range(2, 6):
            yr[n].wait_recv()
    combined = part[pl.ds(q_row, TOK), :].astype(F32)
    if Y > 1:
        combined = combined + y_in[0].astype(F32) + y_in[1].astype(F32)
    inverse_rms = lax.rsqrt(jnp.mean(combined * combined, axis=-1, keepdims=True) + norm_floor)
    hn[...] = combined * inverse_rms * gain_ref[...]

    loads[4].wait()

    def owner(j):
        if X == 1:
            return x
        return jnp.where(j == 0, x_far, jnp.where(j == 1, x_up, jnp.where(j == 2, x_down, x)))

    def shared(j, cc):
        index = slot(owner(j), cc)
        rows = pl.ds(pl.multiple_of(index * R, 8), R)
        return jnp.dot(hn[rows, :].astype(BF16), wo[...], preferred_element_type=F32)

    def d_copy(j):
        return remote(d_out.at[j], d_in.at[j], do_send.at[j], do_recv.at[j], at_x(x, other))

    def for_other(j, carry):
        d_out[j] = shared(j, other).astype(BF16)
        d_copy(j).start()
        return carry

    lax.fori_loop(0, X, for_other, 0)
    left, right = pl.ds(0, cols), pl.ds(cols, cols)
    if X > 1:
        xr = [
            remote(sx.at[0, :, left], x_relay.at[0], xr_send.at[0], xr_recv.at[0], at_x(x_up, c)),
            remote(sx.at[0, :, right], x_relay.at[1], xr_send.at[1], xr_recv.at[1], at_x(x_down, c)),
            remote(sx.at[1, :, right], x_in.at[0, :, right], xr_send.at[2], xr_recv.at[2], at_x(x_up, c)),
            remote(sx.at[2, :, left], x_in.at[1, :, left], xr_send.at[3], xr_recv.at[3], at_x(x_down, c)),
            remote(x_sum.at[0], x_in.at[0, :, left], xr_send.at[4], xr_recv.at[4], at_x(x_up, c)),
            remote(x_sum.at[1], x_in.at[1, :, right], xr_send.at[5], xr_recv.at[5], at_x(x_down, c)),
        ]

    def for_own(j, carry):
        mine = shared(j, c)
        d_copy(j).wait_recv()
        sx[j] = (mine + d_in[j].astype(F32)).astype(BF16)
        if X > 1:

            @pl.when(j == 0)
            def _():
                xr[0].start()
                xr[1].start()

            @pl.when(j == 1)
            def _():
                xr[2].start()

            @pl.when(j == 2)
            def _():
                xr[3].start()

        return carry

    lax.fori_loop(0, X, for_own, 0)
    if X > 1:
        xr[0].wait_recv()
        x_sum[0] = (sx[1, :, 0:cols].astype(F32) + x_relay[0].astype(F32)).astype(BF16)
        xr[4].start()
        xr[1].wait_recv()
        x_sum[1] = (sx[2, :, cols : 2 * cols].astype(F32) + x_relay[1].astype(F32)).astype(BF16)
        xr[5].start()
        for n in range(2, 6):
            xr[n].wait_recv()
        out_ref[...] = (
            sx[3].astype(F32) + x_in[0].astype(F32) + x_in[1].astype(F32)
        ).astype(BF16)
    else:
        out_ref[...] = sx[0]

    if X > 1:
        for copy in xa + xr:
            copy.wait_send()
    for copy in dd:
        copy.wait_send()
    for j in range(X):
        d_copy(j).wait_send()
    if Y > 1:
        for copy in qc + sc + yr:
            copy.wait_send()
    if Z > 1:

        def drain(e, carry):
            s, k = e // 2, lax.rem(e, 2)

            @pl.when(right_goes(z, s, k))
            def _():
                z_copy(True, s, k, right_origin(z, s)).wait_send()

            @pl.when(left_goes(z, s, k))
            def _():
                z_copy(False, s, k, left_origin(z, s)).wait_send()

            return carry

        lax.fori_loop(0, 2 * reach, drain, 0)


def layer(X, Y, Z, activations, query_weight, key_weight, value_weight, out_weight, lambdas, head_gain):
    R, D = activations.shape
    TOK = R * 2 * X
    QT = 256 if (Y * TOK) % 256 == 0 else TOK
    NT = Y * TOK // QT
    half = TOK // 2
    any_space = pl.BlockSpec(memory_space=pl.ANY)
    dma = pltpu.SemaphoreType.DMA
    reach = max(Z // 2, 1)
    return pl.pallas_call(
        functools.partial(fused, X, Y, Z, TOK, D, R, QT),
        out_shape=jax.ShapeDtypeStruct((R, D), BF16),
        in_specs=[any_space] * 5
        + [pl.BlockSpec(memory_space=pltpu.SMEM), pl.BlockSpec(memory_space=pltpu.VMEM)],
        out_specs=pl.BlockSpec(memory_space=pltpu.VMEM),
        scratch_shapes=[
            pltpu.VMEM((2 * X, R, D), BF16),
            pltpu.VMEM((D, 256), BF16),
            pltpu.VMEM((D, 256), BF16),
            pltpu.VMEM((D, 256), BF16),
            pltpu.VMEM((VALUE, D), BF16),
            pltpu.VMEM((TOK, 768), F32),
            pltpu.VMEM((Z, TOK, 512), BF16),
            pltpu.VMEM((Y * TOK, 256), BF16),
            pltpu.VMEM((VALUE, 512), BF16),
            pltpu.VMEM((NT, 2, VALUE, QT), F32),
            pltpu.VMEM((4 * NT, 8, QT), F32),
            pltpu.VMEM((Y * TOK, VALUE), BF16),
            pltpu.VMEM((2, half, VALUE), BF16),
            pltpu.VMEM((2, TOK, VALUE), BF16),
            pltpu.VMEM((2, half, VALUE), BF16),
            pltpu.VMEM((TOK, VALUE), F32),
            pltpu.VMEM((X, R, D), BF16),
            pltpu.VMEM((X, R, D), BF16),
            pltpu.VMEM((X, R, D), BF16),
            pltpu.VMEM((2, R, D // 2), BF16),
            pltpu.VMEM((2, R, D), BF16),
            pltpu.VMEM((2, R, D // 2), BF16),
            dma((5,)),
            dma((3,)), dma((3,)), dma((4,)), dma((4,)), dma((6,)), dma((6,)),
            dma((reach, 2)), dma((reach, 2)), dma((reach, 2)), dma((reach, 2)),
            dma((3,)), dma((3,)), dma((6,)), dma((6,)), dma((X,)), dma((X,)), dma((6,)), dma((6,)),
        ],
        compiler_params=pltpu.CompilerParams(
            collective_id=0, has_side_effects=True, vmem_limit_bytes=60 * 2**20
        ),
    )(
        activations, query_weight, key_weight, value_weight, out_weight, lambdas, head_gain.reshape(1, VALUE)
    )


def build(mesh, Y):
    X = mesh.shape["tp"] // 2
    Z = mesh.shape["sp"] // Y
    in_specs = (
        P(("sp", "tp"), None),
        P(None, "tp"),
        P(None, "tp"),
        P(None, "tp"),
        P("tp", None),
        P("tp"),
        P(),
    )
    out_specs = P(("sp", "tp"), None)
    return jax.shard_map(
        functools.partial(layer, X, Y, Z), mesh=mesh, in_specs=in_specs, out_specs=out_specs, check_vma=False
    )


def solution(mesh):
    return build(mesh, 4)
```
